32 devices in a mesh: st: 4 (over y, x), tp: 8 (over z, core).
Axes of the slice: x: 2, y: 2, z: 4, core: 2. Of those that a mesh axis runs over, the one named last changes fastest.
Arguments:
- tokens: bfloat16 [2048, 4096], P('st', 'tp'), may hold values from -6 to 6
- w_query: bfloat16 [4096, 2048], P(None, 'tp'), may hold values from -0.09375 to 0.09375
- w_key: bfloat16 [4096, 2048], P(None, 'tp'), may hold values from -0.09375 to 0.09375
- w_value: bfloat16 [4096, 4096], P(None, 'tp'), may hold values from -0.09375 to 0.09375
- w_mem_query: bfloat16 [4096, 2048], P(None, 'tp'), may hold values from -0.09375 to 0.09375
- w_mem_key: bfloat16 [4096, 2048], P(None, 'tp'), may hold values from -0.09375 to 0.09375
- w_mem_value: bfloat16 [4096, 2048], P(None, 'tp'), may hold values from -0.09375 to 0.09375
- w_gate: bfloat16 [4096, 16], P(None, 'tp'), may hold values from -0.09375 to 0.09375
- w_lift: bfloat16 [16, 128, 256], P('tp'), may hold values from -4 to 4
- decay_rate: float32 [16], P('tp'), may hold values from 0.000390625 to 0.1
- store: bfloat16 [512, 64, 4096], P('st', None, 'tp'), may hold values from -6 to 6
- passage_ids: int32 [16, 2], P('st'), may hold values from 0 to 511, as said below
Outputs:
- mixed: bfloat16 [2048, 4096], P('st', 'tp')
The draws below stay inside these ranges and needn't reach their ends.
Inputs may be any that keep to these rules, and one draw needn't show every extreme that they name: `passage_ids`: passage p is held by index p // 128 of st. Among the requests of the rows of one device along st, at most 4 name passages held by one index of st, and in every draw some index receives exactly 4 of them.
All inputs are finite; a program needn't handle non-finite values.
Results may differ from the reference program's by a relative error of at most 0.0095.
Values may be sent and summed in bfloat16 or wider, within the bound.
No kernel may reach another device: no remote copies, remote signals or barrier semaphores. Data moves between devices by JAX's collectives and lax.ppermute only.
A program may use at most 64 MiB of HBM per device.

```python
import jax
import jax.numpy as jnp
from jax import lax

D = 4096
HEADS = 16
KEY_DIM = 128
VALUE_DIM = 256
MEM_DIM = 128
TOK_DEV = 512
SEQ_LEN = 512
RET_BLOCK = 64
BLOCK = 128
PICKS = 2
PASS_ROWS = 64
PASS_DEV = 128
CAP = 4
TOKENS = 2048
BLOCKS = 16
PASSAGES = 512
N_ST = 4


def draw_decay_rate(key, part):
    pick_key, slow_key, fast_key = jax.random.split(key, 3)
    quick = jax.random.uniform(pick_key, (HEADS,)) < 0.5
    slow_rate = jnp.exp(jax.random.uniform(slow_key, (HEADS,), minval=jnp.log(0.2 / SEQ_LEN), maxval=jnp.log(2.0 / SEQ_LEN)))
    fast_rate = jnp.exp(jax.random.uniform(fast_key, (HEADS,), minval=jnp.log(0.03), maxval=jnp.log(0.1)))
    return jnp.where(quick, fast_rate, slow_rate).astype(jnp.float32)


def draw_passage_ids(key, part):
    requests = TOK_DEV // BLOCK * PICKS
    slot_count = N_ST * CAP
    owners = jnp.repeat(jnp.arange(N_ST, dtype=jnp.int32), CAP)
    copies = jnp.tile(jnp.arange(CAP, dtype=jnp.int32), N_ST)

    def one_device(device):
        device_key = jax.random.fold_in(key, device)
        rank_key, shuffle_key, first_key, second_key = jax.random.split(device_key, 4)
        before = (device + N_ST - 1) % N_ST
        across = (device + N_ST // 2) % N_ST
        priority = jnp.where(owners == before, 0, jnp.where((owners == across) & (copies == 0), 1, 2))
        noise_rank = jax.random.randint(rank_key, (slot_count,), 0, 1 << 12)
        scores = priority * (1 << 24) + noise_rank * slot_count + jnp.arange(slot_count, dtype=jnp.int32)
        chosen = owners[jnp.argsort(scores)[:requests]]
        chosen = chosen[jax.random.permutation(shuffle_key, requests)]
        first_pick = jax.random.randint(first_key, (requests,), 0, PASS_DEV)
        second_pick = jax.random.randint(second_key, (requests,), 0, PASS_DEV)
        return chosen * PASS_DEV + jnp.minimum(first_pick, second_pick)
    drawn = jax.vmap(one_device)(jnp.arange(N_ST, dtype=jnp.int32))
    return drawn.reshape(BLOCKS, PICKS).astype(jnp.int32)


def block_scale(stream_key, extent, cuts, least, top_value):
    def one(dim, shards_of):
        heights = jax.random.uniform(jax.random.fold_in(jax.random.fold_in(stream_key, 6), dim), (shards_of,), jnp.float32, least / len(cuts), top_value / len(cuts))
        return jnp.repeat(jnp.exp(heights), extent[dim] // shards_of).reshape((-1,) + (1,) * (len(extent) - dim - 1))

    factor_of = one(*cuts[0])
    for cut in cuts[1:]:
        factor_of = factor_of * one(*cut)
    return factor_of


def noise(key, dims, scale, limit, cuts=(), held_as=jnp.bfloat16):
    entries = scale * jax.random.normal(key, dims, jnp.float32)
    if cuts:
        entries = entries * block_scale(key, dims, cuts, -0.22, 0.18)
    return jnp.clip(entries, -limit, limit).astype(held_as)


def setup_inputs(seed: int = 0) -> dict:
    streams_of = jax.random.split(jax.random.key(seed), 13)
    return {
        "tokens": noise(streams_of[0], (TOKENS, D), 1.0, 6.0, ((0, 4), (1, 8))),
        "w_query": noise(streams_of[1], (D, HEADS * KEY_DIM), D ** -0.5, 0.09375, ((1, 8),)),
        "w_key": noise(streams_of[2], (D, HEADS * KEY_DIM), D ** -0.5, 0.09375, ((1, 8),)),
        "w_value": noise(streams_of[3], (D, HEADS * VALUE_DIM), D ** -0.5, 0.09375, ((1, 8),)),
        "w_mem_query": noise(streams_of[4], (D, HEADS * MEM_DIM), D ** -0.5, 0.09375, ((1, 8),)),
        "w_mem_key": noise(streams_of[5], (D, HEADS * MEM_DIM), D ** -0.5, 0.09375, ((1, 8),)),
        "w_mem_value": noise(streams_of[6], (D, HEADS * MEM_DIM), D ** -0.5, 0.09375, ((1, 8),)),
        "w_gate": noise(streams_of[7], (D, HEADS), D ** -0.5, 0.09375, ((1, 8),)),
        "w_lift": noise(streams_of[8], (HEADS, MEM_DIM, VALUE_DIM), 0.7, 4.0, ((0, 8),)),
        "decay_rate": draw_decay_rate(jax.random.fold_in(streams_of[12], 71), 0),
        "store": noise(streams_of[10], (PASSAGES, PASS_ROWS, D), 1.0, 6.0, ((0, 4), (2, 8))),
        "passage_ids": draw_passage_ids(jax.random.fold_in(streams_of[12], 71), 0),
    }


norm_eps = 1e-06
rope_base = 10000.0

def rotate(values, positions):
    half_dim = values.shape[-1] // 2
    inverse = rope_base ** (-jnp.arange(half_dim, dtype=jnp.float32) / half_dim)
    angles = positions.astype(jnp.float32)[:, None] * inverse[None, :]
    cosine = jnp.cos(angles)[:, None, :]
    sine_table = jnp.sin(angles)[:, None, :]
    first_half = values[..., :half_dim]
    second_half = values[..., half_dim:]
    return jnp.concatenate([first_half * cosine - second_half * sine_table, first_half * sine_table + second_half * cosine], axis=-1)

def head_norm(values):
    return values * lax.rsqrt(lax.optimization_barrier(jnp.mean(values * values, axis=-1, keepdims=True)) + norm_eps)

def group_norm(values):
    centred = values - lax.optimization_barrier(jnp.mean(values, axis=-1, keepdims=True))
    return centred * lax.rsqrt(lax.optimization_barrier(jnp.mean(centred * centred, axis=-1, keepdims=True)) + norm_eps)

def retention(ret_query, ret_key, ret_value, rates, block_len):
    tokens_all, head_count, key_dim = ret_query.shape
    value_dim = ret_value.shape[-1]
    sequences = tokens_all // SEQ_LEN
    block_count = SEQ_LEN // block_len

    def blocked(array):
        shaped = array.astype(jnp.float32).reshape(sequences, block_count, block_len, head_count, array.shape[-1])
        return jnp.swapaxes(shaped, 0, 1)
    log_decay = -rates.astype(jnp.float32)
    offsets = jnp.arange(block_len, dtype=jnp.float32)
    decay_query = jnp.exp(log_decay[None, :] * (offsets[:, None] + 1.0))
    distance = offsets[:, None] - offsets[None, :]
    decay_mask = jnp.where(distance[None] >= 0.0, jnp.exp(log_decay[:, None, None] * jnp.maximum(distance, 0.0)[None]), 0.0)
    decay_key = jnp.exp(log_decay[None, :] * (block_len - 1.0 - offsets[:, None]))
    decay_block = jnp.exp(log_decay * block_len)
    highest = lax.Precision.HIGHEST

    def advance(memory_state, pieces):
        query_block, key_block, value_block = pieces
        carried = jnp.einsum('slhk,shkv->slhv', query_block, memory_state, precision=highest) * decay_query[None, :, :, None]
        scores = jnp.einsum('slhk,smhk->shlm', query_block, key_block, precision=highest) * decay_mask[None]
        within = jnp.einsum('shlm,smhv->slhv', scores, value_block, precision=highest)
        weighted = key_block * decay_key[None, :, :, None]
        memory_state = decay_block[None, :, None, None] * memory_state + jnp.einsum('slhk,slhv->shkv', weighted, value_block, precision=highest)
        return (memory_state, carried + within)
    initial = jnp.zeros((sequences, head_count, key_dim, value_dim), jnp.float32)
    _, outputs = lax.scan(advance, initial, (blocked(ret_query), blocked(ret_key), blocked(ret_value)))
    return jnp.swapaxes(outputs, 0, 1).reshape(tokens_all, head_count, value_dim)

def reference(tokens, w_query, w_key, w_value, w_mem_query, w_mem_key, w_mem_value, w_gate, w_lift, decay_rate, store, passage_ids):
    total_rows = tokens.shape[0]
    head_count = decay_rate.shape[0]
    highest = lax.Precision.HIGHEST
    features = tokens.astype(jnp.float32)
    row_scale = lax.rsqrt(lax.optimization_barrier(jnp.mean(features * features, axis=1, keepdims=True)) + norm_eps)
    positions = jnp.arange(total_rows, dtype=jnp.int32) % SEQ_LEN

    def project(weight):
        return jnp.dot(tokens, weight, preferred_element_type=jnp.float32)
    ret_query = rotate((project(w_query) * row_scale).reshape(total_rows, head_count, KEY_DIM), positions).astype(jnp.bfloat16)
    ret_key = (rotate((project(w_key) * row_scale).reshape(total_rows, head_count, KEY_DIM), positions) * KEY_DIM ** (-0.5)).astype(jnp.bfloat16)
    ret_value = (project(w_value) * row_scale).astype(jnp.bfloat16).reshape(total_rows, head_count, VALUE_DIM)
    mem_query = head_norm(project(w_mem_query).reshape(total_rows, head_count, MEM_DIM)).astype(jnp.bfloat16)
    gate_value = jax.nn.sigmoid(project(w_gate) * row_scale)
    ret_norm = group_norm(retention(ret_query, ret_key, ret_value, decay_rate, RET_BLOCK))

    def passage_rows(ident):
        passage = lax.dynamic_index_in_dim(store, ident, 0, keepdims=False)
        key_part = head_norm(jnp.dot(passage, w_mem_key, preferred_element_type=jnp.float32).reshape(PASS_ROWS, head_count, MEM_DIM))
        value_part = jnp.dot(passage, w_mem_value, preferred_element_type=jnp.float32).reshape(PASS_ROWS, head_count, MEM_DIM)
        return (key_part.astype(jnp.bfloat16), value_part.astype(jnp.bfloat16))
    pass_key, pass_value = lax.map(passage_rows, passage_ids.reshape(-1).astype(jnp.int32))
    block_count, picks = passage_ids.shape
    query_blocks = mem_query.reshape(block_count, BLOCK, head_count, MEM_DIM)
    key_blocks = pass_key.reshape(block_count, picks, PASS_ROWS, head_count, MEM_DIM)
    value_blocks = pass_value.reshape(block_count, picks, PASS_ROWS, head_count, MEM_DIM)

    def attend(pieces):
        query_block, key_block, value_block = pieces
        scores = jnp.einsum('thd,prhd->hptr', query_block.astype(jnp.float32), key_block.astype(jnp.float32), precision=highest) * MEM_DIM ** (-0.5)
        exponent = jnp.exp(scores)
        mass_sum = lax.optimization_barrier(jnp.sum(exponent, axis=3))
        rounded = lax.optimization_barrier(exponent.astype(jnp.bfloat16)).astype(jnp.float32)
        partial_value = jnp.einsum('hptr,prhd->pthd', rounded, value_block.astype(jnp.float32), precision=highest)
        partial_value = lax.optimization_barrier(partial_value.astype(jnp.bfloat16)).astype(jnp.float32)
        summed = lax.optimization_barrier(jnp.sum(partial_value, axis=0))
        return summed / jnp.swapaxes(lax.optimization_barrier(jnp.sum(mass_sum, axis=1)), 0, 1)[:, :, None]
    mem_out = lax.map(attend, (query_blocks, key_blocks, value_blocks)).reshape(total_rows, head_count, MEM_DIM).astype(jnp.bfloat16)
    mem_lift = jnp.einsum('thd,hde->the', mem_out.astype(jnp.float32), w_lift.astype(jnp.float32), precision=highest)
    mixed = (ret_norm + gate_value[:, :, None] * mem_lift).astype(jnp.bfloat16)
    return mixed.reshape(total_rows, head_count * VALUE_DIM)
```

```python
import functools

import jax
import jax.numpy as jnp
from jax import lax
from jax.experimental import pallas as pl
from jax.experimental.pallas import tpu as pltpu
from jax.sharding import PartitionSpec as P


D = 4096
KEY_DIM = 128
VALUE_DIM = 256
MEM_DIM = 128
SEQ_LEN = 512
BLOCK = 128
PASS_ROWS = 64
LANES = 128
TILE = 128

norm_eps = 1e-06
rope_base = 10000.0


f32 = jnp.float32
bf16 = jnp.bfloat16
ANY = pl.BlockSpec(memory_space=pl.ANY)
SMEM = pl.BlockSpec(memory_space=pltpu.SMEM)
VMEM = pl.BlockSpec(memory_space=pltpu.VMEM)


def rotary_tables(rows):
    half_dim = KEY_DIM // 2
    positions = (jnp.arange(rows, dtype=jnp.int32) % SEQ_LEN).astype(f32)
    inverse = rope_base ** (-jnp.arange(half_dim, dtype=f32) / half_dim)
    angles = positions[:, None] * inverse[None, :]
    cosine = jnp.cos(angles)
    sine = jnp.sin(angles)
    return (
        jnp.concatenate([cosine, cosine], axis=1),
        jnp.concatenate([-sine, sine], axis=1),
    )


def dot(a, b):
    return jnp.dot(a, b, preferred_element_type=f32)


def ring_gather(halves, ring_size, core_count):
    total = ring_size * core_count
    half = halves[0].shape[0]
    me = lax.axis_index("tp")

    def step(value, chips):
        moves = [(i, (i + chips * core_count) % total) for i in range(total)]
        return lax.ppermute(value, "tp", moves)

    def swap(value):
        moves = [(i, i + 1 - 2 * (i % 2)) for i in range(total)]
        return lax.ppermute(value, "tp", moves)

    held = [(halves[0], 0, 0), (halves[1], 0, half)]
    right = left = halves
    far = ring_size // 2
    for distance in range(1, far):
        right_top, left_bottom = step(right[0], 1), step(left[1], -1)
        right_bottom, left_top = step(right[1], 1), step(left[0], -1)
        right, left = (right_top, right_bottom), (left_top, left_bottom)
        held += [
            (right_top, -distance, 0),
            (left_bottom, distance, half),
            (right_bottom, -distance, half),
            (left_top, distance, 0),
        ]
    if ring_size > 1:
        held += [(step(right[0], 1), far, 0), (step(left[1], -1), far, half)]
    parts = []
    chips = []
    for value, offset, first in held:
        offset = offset % ring_size
        if offset not in chips:
            chips.append(offset)
        slot = chips.index(offset) * core_count
        parts.append((value, slot, first))
        parts.append((swap(value), slot + 1, first))
    order = []
    core = me & 1
    for offset in chips:
        base = ((me >> 1) + offset) & (ring_size - 1)
        order += [base * core_count + core, base * core_count + 1 - core]
    return parts, jnp.stack(order)


def project_kernel(places, heads, *refs):
    count = len(places)
    order, rates = refs[:2]
    parts = refs[2 : 2 + count]
    weights = refs[2 + count : 7 + count]
    cos_ref, sin_ref, norm_out, query_out, gate_out, xs, ws, acc, sem_x, sem_w = refs[7 + count :]
    slots = ws.shape[0]
    depth = ws.shape[1]
    rows = xs.shape[1]
    copies = [[] for _ in range(slots)]
    for p, (slot, first) in enumerate(places):
        extent = parts[p].shape[0]
        copies[slot].append(
            pltpu.make_async_copy(parts[p], xs.at[slot, pl.ds(first, extent)], sem_x.at[p])
        )
    for slot in range(slots):
        start = 0
        row = pl.multiple_of(order[slot] * depth, depth)
        for w, weight in enumerate(weights):
            width = weight.shape[1]
            copies[slot].append(
                pltpu.make_async_copy(
                    weight.at[pl.ds(row, depth)],
                    ws.at[slot, :, pl.ds(start, width)],
                    sem_w.at[slot, w],
                )
            )
            start += width
    for group in copies:
        for copy in group:
            copy.start()
    squares = jnp.zeros((rows, LANES), f32)
    for slot in range(slots):
        for copy in copies[slot]:
            copy.wait()
        x = xs[slot]
        wide = x.astype(f32)
        wide = wide * wide
        for lane in range(depth // LANES):
            squares += wide[:, lane * LANES : (lane + 1) * LANES]
        if slot == 0:
            acc[...] = dot(x, ws[slot])
        else:
            acc[...] += dot(x, ws[slot])
    row_scale = lax.rsqrt(jnp.sum(squares, axis=1, keepdims=True) / D + norm_eps)
    key_at = heads * KEY_DIM
    value_at = 2 * heads * KEY_DIM
    mem_at = value_at + heads * VALUE_DIM
    gate_at = mem_at + heads * MEM_DIM
    gate_raw = acc[:, gate_at : gate_at + LANES] * row_scale
    gate_out[...] = jax.nn.sigmoid(gate_raw)
    cosine = cos_ref[...]
    sine = sin_ref[...]
    for h in range(heads):
        z = acc[:, mem_at + h * MEM_DIM : mem_at + (h + 1) * MEM_DIM]
        z = z * lax.rsqrt(jnp.mean(z * z, axis=1, keepdims=True) + norm_eps)
        query_out[:, h * MEM_DIM : (h + 1) * MEM_DIM] = z.astype(bf16)
        q = acc[:, h * KEY_DIM : (h + 1) * KEY_DIM] * row_scale
        q = (q * cosine + pltpu.roll(q, KEY_DIM // 2, 1) * sine).astype(bf16)
        k = acc[:, key_at + h * KEY_DIM : key_at + (h + 1) * KEY_DIM] * row_scale
        k = (k * cosine + pltpu.roll(k, KEY_DIM // 2, 1) * sine) * KEY_DIM ** (-0.5)
        k = k.astype(bf16)
        v = acc[:, value_at + h * VALUE_DIM : value_at + (h + 1) * VALUE_DIM] * row_scale
        v = v.astype(bf16)
        for first in range(0, rows, TILE):
            base = first // SEQ_LEN * SEQ_LEN
            end = first + TILE
            scores = lax.dot_general(
                q[first:end], k[base:end], (((1,), (1,)), ((), ())), preferred_element_type=f32
            )
            shape = scores.shape
            gap = (
                lax.broadcasted_iota(jnp.int32, shape, 0)
                - lax.broadcasted_iota(jnp.int32, shape, 1)
                + (first - base)
            )
            decay = jnp.exp(-rates[h] * jnp.maximum(gap, 0).astype(f32))
            scores = jnp.where(gap >= 0, scores * decay, 0.0)
            upper = scores.astype(bf16)
            lower = (scores - upper.astype(f32)).astype(bf16)
            out = dot(upper, v[base:end]) + dot(lower, v[base:end])
            out = out - jnp.mean(out, axis=1, keepdims=True)
            out = out * lax.rsqrt(jnp.mean(out * out, axis=1, keepdims=True) + norm_eps)
            norm_out[first:end, h * VALUE_DIM : (h + 1) * VALUE_DIM] = out


def project(parts, order, weights, rates, tables):
    heads = rates.shape[0]
    places = tuple((slot, first) for _, slot, first in parts)
    rows, depth = 2 * parts[0][0].shape[0], parts[0][0].shape[1]
    slots = order.shape[0]
    width = sum(w.shape[1] for w in weights)
    return pl.pallas_call(
        functools.partial(project_kernel, places, heads),
        out_shape=(
            jax.ShapeDtypeStruct((rows, heads * VALUE_DIM), f32),
            jax.ShapeDtypeStruct((rows, heads * MEM_DIM), bf16),
            jax.ShapeDtypeStruct((rows, LANES), f32),
        ),
        in_specs=[SMEM, SMEM] + [ANY] * (len(parts) + len(weights)) + [VMEM, VMEM],
        out_specs=(VMEM, VMEM, VMEM),
        scratch_shapes=[
            pltpu.VMEM((slots, rows, depth), bf16),
            pltpu.VMEM((slots, depth, width), bf16),
            pltpu.VMEM((rows, width), f32),
            pltpu.SemaphoreType.DMA((len(parts),)),
            pltpu.SemaphoreType.DMA((slots, len(weights))),
        ],
        compiler_params=pltpu.CompilerParams(vmem_limit_bytes=40 * 1024 * 1024),
        cost_estimate=pl.CostEstimate(
            flops=2 * rows * depth * slots * width, bytes_accessed=0, transcendentals=0
        ),
        name="project_retain",
    )(order, rates, *[p[0] for p in parts], *weights, *tables)


def fetch_kernel(index, store, *refs):
    outs, sems = refs[:-1], refs[-1]
    copies = []
    for out in outs:
        for i in range(out.shape[0]):
            at = len(copies)
            copies.append(pltpu.make_async_copy(store.at[index[at]], out.at[i], sems.at[at]))
    for copy in copies:
        copy.start()
    for copy in copies:
        copy.wait()


def fetch(store, index, peers):
    count = index.shape[0]
    shape = jax.ShapeDtypeStruct((count // peers,) + store.shape[1:], store.dtype)
    return pl.pallas_call(
        fetch_kernel,
        out_shape=(shape,) * peers,
        in_specs=[SMEM, ANY],
        out_specs=(VMEM,) * peers,
        scratch_shapes=[pltpu.SemaphoreType.DMA((count,))],
        name="fetch_rows",
    )(index, store)


def compact_kernel(source, index, store, *refs):
    arrived = refs[:-3]
    halves, sems = refs[-3:-1], refs[-1]
    half = halves[0].shape[0]
    for i in range(2 * half):
        out = halves[i // half].at[i % half]
        for k, ref in enumerate((store,) + tuple(arrived)):

            @pl.when(source[i] == k)
            def _():
                pltpu.make_async_copy(ref.at[index[i]], out, sems.at[i]).start()

    for i in range(2 * half):
        out = halves[i // half].at[i % half]
        pltpu.make_async_copy(store.at[0], out, sems.at[i]).wait()


def compact(store, arrived, source, index):
    count = index.shape[0]
    shape = jax.ShapeDtypeStruct((count // 2,) + store.shape[1:], store.dtype)
    return pl.pallas_call(
        compact_kernel,
        out_shape=(shape, shape),
        in_specs=[SMEM, SMEM] + [ANY] * (1 + len(arrived)),
        out_specs=(VMEM, VMEM),
        scratch_shapes=[pltpu.SemaphoreType.DMA((count,))],
        name="compact_rows",
    )(source, index, store, *arrived)


def passage_kernel(places, heads, picks, *refs):
    count = len(places)
    order = refs[0]
    parts = refs[1 : 1 + count]
    weights = refs[1 + count : 3 + count]
    query, gate, norm, lift, out, xs, ws, acc, sem_x, sem_w = refs[3 + count :]
    slots = ws.shape[0]
    depth = ws.shape[1]
    width = heads * MEM_DIM
    copies = [[] for _ in range(slots)]
    for p, (slot, first) in enumerate(places):
        extent = parts[p].shape[0]
        copies[slot].append(
            pltpu.make_async_copy(parts[p], xs.at[slot, pl.ds(first, extent)], sem_x.at[p])
        )
    for slot in range(slots):
        row = pl.multiple_of(order[slot] * depth, depth)
        for w, weight in enumerate(weights):
            copies[slot].append(
                pltpu.make_async_copy(
                    weight.at[pl.ds(row, depth)],
                    ws.at[slot, :, pl.ds(w * width, width)],
                    sem_w.at[slot, w],
                )
            )
    for group in copies:
        for copy in group:
            copy.start()
    for slot in range(slots):
        for copy in copies[slot]:
            copy.wait()
        if slot == 0:
            acc[...] = dot(xs[slot], ws[slot])
        else:
            acc[...] += dot(xs[slot], ws[slot])
    block_rows = picks * PASS_ROWS
    for h in range(heads):
        lo, hi = h * MEM_DIM, (h + 1) * MEM_DIM
        k = acc[:, lo:hi]
        k = k * lax.rsqrt(jnp.mean(k * k, axis=1, keepdims=True) + norm_eps)
        k = k.astype(bf16)
        v = acc[:, width + lo : width + hi].astype(bf16)
        for b in range(query.shape[0] // BLOCK):
            top, end = b * BLOCK, (b + 1) * BLOCK
            q = query[top:end, lo:hi]
            first, last = b * block_rows, (b + 1) * block_rows
            scores = lax.dot_general(
                q, k[first:last], (((1,), (1,)), ((), ())), preferred_element_type=f32
            )
            exponent = jnp.exp(scores * MEM_DIM ** (-0.5))
            mass = jnp.sum(exponent, axis=1, keepdims=True)
            summed = dot(exponent.astype(bf16), v[first:last])
            mem_out = (summed / mass).astype(bf16)
            lifted = dot(mem_out, lift[h])
            cols = slice(h * VALUE_DIM, (h + 1) * VALUE_DIM)
            out[top:end, cols] = (
                norm[top:end, cols] + gate[top:end, h : h + 1] * lifted
            ).astype(bf16)


def passages(parts, order, weights, query, gate, norm, lift, picks):
    heads = lift.shape[0]
    places = tuple((slot, first) for _, slot, first in parts)
    rows, depth = 2 * parts[0][0].shape[0], parts[0][0].shape[1]
    slots = order.shape[0]
    width = sum(w.shape[1] for w in weights)
    return pl.pallas_call(
        functools.partial(passage_kernel, places, heads, picks),
        out_shape=jax.ShapeDtypeStruct(norm.shape, bf16),
        in_specs=[SMEM] + [ANY] * (len(parts) + len(weights)) + [VMEM] * 4,
        out_specs=VMEM,
        scratch_shapes=[
            pltpu.VMEM((slots, rows, depth), bf16),
            pltpu.VMEM((slots, depth, width), bf16),
            pltpu.VMEM((rows, width), f32),
            pltpu.SemaphoreType.DMA((len(parts),)),
            pltpu.SemaphoreType.DMA((slots, len(weights))),
        ],
        compiler_params=pltpu.CompilerParams(vmem_limit_bytes=32 * 1024 * 1024),
        cost_estimate=pl.CostEstimate(
            flops=2 * rows * depth * slots * width, bytes_accessed=0, transcendentals=0
        ),
        name="passage_mix",
    )(order, *[p[0] for p in parts], *weights, query, gate, norm, lift)


def per_device(
    ring_size,
    core_count,
    tokens,
    w_query,
    w_key,
    w_value,
    w_mem_query,
    w_mem_key,
    w_mem_value,
    w_gate,
    w_lift,
    decay_rate,
    store,
    passage_ids,
):
    block_count, picks = passage_ids.shape
    request_count = block_count * picks
    group_count = lax.axis_size("st")
    capacity = max(1, 2 * request_count // group_count)
    held_count = store.shape[0]
    mine = lax.axis_index("st")

    def exchange(value, k):
        return lax.ppermute(value, "st", [(i, i ^ k) for i in range(group_count)])

    wanted = passage_ids.reshape(request_count)
    owners = wanted // held_count
    held_index = wanted % held_count
    ordinal = jnp.arange(request_count, dtype=jnp.int32)
    earlier = (owners[:, None] == owners[None, :]) & (ordinal[None, :] < ordinal[:, None])
    slot_index = jnp.sum(earlier.astype(jnp.int32), axis=1)
    source = owners ^ mine
    place = source * capacity + slot_index
    selector = (
        place[:, None] == jnp.arange(group_count * capacity, dtype=jnp.int32)[None, :]
    ).astype(jnp.int32)
    outgoing = jnp.sum(selector * held_index[:, None], axis=0).reshape(group_count, capacity)
    incoming = [exchange(outgoing[k], k) for k in range(1, group_count)]

    half = tokens.shape[0] // 2
    token_halves = (tokens[:half], tokens[half:])
    token_parts, order = ring_gather(token_halves, ring_size, core_count)

    fetched = fetch(store, jnp.concatenate(incoming), group_count - 1)
    arrived = [exchange(fetched[k - 1], k) for k in range(1, group_count)]
    rows_at = jnp.where(source == 0, held_index, slot_index)
    own_rows = compact(store, arrived, source, rows_at)
    own_rows = [x.reshape(-1, store.shape[2]) for x in own_rows]
    row_parts, _ = ring_gather(tuple(own_rows), ring_size, core_count)

    gate_wide = jnp.pad(w_gate, ((0, 0), (0, LANES - w_gate.shape[1])))
    tables = rotary_tables(tokens.shape[0])
    norm, query, gate = project(
        token_parts,
        order,
        (w_query, w_key, w_value, w_mem_query, gate_wide),
        decay_rate,
        tables,
    )
    return passages(
        row_parts, order, (w_mem_key, w_mem_value), query, gate, norm, w_lift, picks
    )


def solution(mesh):
    in_specs = (
        P("st", "tp"),
        P(None, "tp"),
        P(None, "tp"),
        P(None, "tp"),
        P(None, "tp"),
        P(None, "tp"),
        P(None, "tp"),
        P(None, "tp"),
        P("tp", None, None),
        P("tp"),
        P("st", None, "tp"),
        P("st", None),
    )
    out_specs = P("st", "tp")
    core_count = 2
    ring_size = mesh.shape["tp"] // core_count
    body = functools.partial(per_device, ring_size, core_count)

    return jax.shard_map(
        body,
        mesh=mesh,
        in_specs=in_specs,
        out_specs=out_specs,
        check_vma=False,
    )
```

```python
import functools

import jax
import jax.numpy as jnp
from jax import lax
from jax.experimental import pallas as pl
from jax.experimental.pallas import tpu as pltpu
from jax.sharding import PartitionSpec as P


D = 4096
KEY_DIM = 128
VALUE_DIM = 256
MEM_DIM = 128
SEQ_LEN = 512
BLOCK = 128
PASS_ROWS = 64
LANES = 128
TILE = 128

norm_eps = 1e-06
rope_base = 10000.0


f32 = jnp.float32
bf16 = jnp.bfloat16
ANY = pl.BlockSpec(memory_space=pl.ANY)
SMEM = pl.BlockSpec(memory_space=pltpu.SMEM)
VMEM = pl.BlockSpec(memory_space=pltpu.VMEM)
HBM = pl.BlockSpec(memory_space=pltpu.HBM)


def rotary_tables(rows):
    half_dim = KEY_DIM // 2
    positions = (jnp.arange(rows, dtype=jnp.int32) % SEQ_LEN).astype(f32)
    inverse = rope_base ** (-jnp.arange(half_dim, dtype=f32) / half_dim)
    angles = positions[:, None] * inverse[None, :]
    cosine = jnp.cos(angles)
    sine = jnp.sin(angles)
    return (
        jnp.concatenate([cosine, cosine], axis=1),
        jnp.concatenate([-sine, sine], axis=1),
    )


def dot(a, b):
    return jnp.dot(a, b, preferred_element_type=f32)


def ring_gather(halves, ring_size, core_count):
    total = ring_size * core_count
    half = halves[0].shape[0]
    me = lax.axis_index("tp")

    def step(value, chips):
        moves = [(i, (i + chips * core_count) % total) for i in range(total)]
        return lax.ppermute(value, "tp", moves)

    def swap(value):
        moves = [(i, i + 1 - 2 * (i % 2)) for i in range(total)]
        return lax.ppermute(value, "tp", moves)

    held = [(halves[0], 0, 0), (halves[1], 0, half)]
    right = left = halves
    far = ring_size // 2
    for distance in range(1, far):
        right_top, left_bottom = step(right[0], 1), step(left[1], -1)
        right_bottom, left_top = step(right[1], 1), step(left[0], -1)
        right, left = (right_top, right_bottom), (left_top, left_bottom)
        held += [
            (right_top, -distance, 0),
            (left_bottom, distance, half),
            (right_bottom, -distance, half),
            (left_top, distance, 0),
        ]
    if ring_size > 1:
        held += [(step(right[0], 1), far, 0), (step(left[1], -1), far, half)]
    parts = []
    chips = []
    for value, offset, first in held:
        offset = offset % ring_size
        if offset not in chips:
            chips.append(offset)
        slot = chips.index(offset) * core_count
        parts.append((value, slot, first))
        parts.append((swap(value), slot + 1, first))
    order = []
    core = me & 1
    for offset in chips:
        base = ((me >> 1) + offset) & (ring_size - 1)
        order += [base * core_count + core, base * core_count + 1 - core]
    return parts, jnp.stack(order)


def project_kernel(places, heads, *refs):
    count = len(places)
    order, rates = refs[:2]
    parts = refs[2 : 2 + count]
    weights = refs[2 + count : 7 + count]
    cos_ref, sin_ref, norm_out, query_out, gate_out, xs, ws, acc, sem_x, sem_w = refs[7 + count :]
    slots = ws.shape[0]
    depth = ws.shape[1]
    rows = xs.shape[1]
    copies = [[] for _ in range(slots)]
    for p, (slot, first) in enumerate(places):
        extent = parts[p].shape[0]
        copies[slot].append(
            pltpu.make_async_copy(parts[p], xs.at[slot, pl.ds(first, extent)], sem_x.at[p])
        )
    for slot in range(slots):
        start = 0
        row = pl.multiple_of(order[slot] * depth, depth)
        for w, weight in enumerate(weights):
            width = weight.shape[1]
            copies[slot].append(
                pltpu.make_async_copy(
                    weight.at[pl.ds(row, depth)],
                    ws.at[slot, :, pl.ds(start, width)],
                    sem_w.at[slot, w],
                )
            )
            start += width
    for group in copies:
        for copy in group:
            copy.start()
    squares = jnp.zeros((rows, LANES), f32)
    for slot in range(slots):
        for copy in copies[slot]:
            copy.wait()
        x = xs[slot]
        wide = x.astype(f32)
        wide = wide * wide
        for lane in range(depth // LANES):
            squares += wide[:, lane * LANES : (lane + 1) * LANES]
        if slot == 0:
            acc[...] = dot(x, ws[slot])
        else:
            acc[...] += dot(x, ws[slot])
    row_scale = lax.rsqrt(jnp.sum(squares, axis=1, keepdims=True) / D + norm_eps)
    key_at = heads * KEY_DIM
    value_at = 2 * heads * KEY_DIM
    mem_at = value_at + heads * VALUE_DIM
    gate_at = mem_at + heads * MEM_DIM
    gate_raw = acc[:, gate_at : gate_at + LANES] * row_scale
    gate_out[...] = jax.nn.sigmoid(gate_raw)
    cosine = cos_ref[...]
    sine = sin_ref[...]
    for h in range(heads):
        z = acc[:, mem_at + h * MEM_DIM : mem_at + (h + 1) * MEM_DIM]
        z = z * lax.rsqrt(jnp.mean(z * z, axis=1, keepdims=True) + norm_eps)
        query_out[:, h * MEM_DIM : (h + 1) * MEM_DIM] = z.astype(bf16)
        q = acc[:, h * KEY_DIM : (h + 1) * KEY_DIM] * row_scale
        q = (q * cosine + pltpu.roll(q, KEY_DIM // 2, 1) * sine).astype(bf16)
        k = acc[:, key_at + h * KEY_DIM : key_at + (h + 1) * KEY_DIM] * row_scale
        k = (k * cosine + pltpu.roll(k, KEY_DIM // 2, 1) * sine) * KEY_DIM ** (-0.5)
        k = k.astype(bf16)
        v = acc[:, value_at + h * VALUE_DIM : value_at + (h + 1) * VALUE_DIM] * row_scale
        v = v.astype(bf16)
        for first in range(0, rows, TILE):
            base = first // SEQ_LEN * SEQ_LEN
            end = first + TILE
            scores = lax.dot_general(
                q[first:end], k[base:end], (((1,), (1,)), ((), ())), preferred_element_type=f32
            )
            shape = scores.shape
            gap = (
                lax.broadcasted_iota(jnp.int32, shape, 0)
                - lax.broadcasted_iota(jnp.int32, shape, 1)
                + (first - base)
            )
            decay = jnp.exp(-rates[h] * jnp.maximum(gap, 0).astype(f32))
            scores = jnp.where(gap >= 0, scores * decay, 0.0)
            upper = scores.astype(bf16)
            lower = (scores - upper.astype(f32)).astype(bf16)
            out = dot(upper, v[base:end]) + dot(lower, v[base:end])
            out = out - jnp.mean(out, axis=1, keepdims=True)
            out = out * lax.rsqrt(jnp.mean(out * out, axis=1, keepdims=True) + norm_eps)
            norm_out[first:end, h * VALUE_DIM : (h + 1) * VALUE_DIM] = out


def project(parts, order, weights, rates, tables):
    heads = rates.shape[0]
    places = tuple((slot, first) for _, slot, first in parts)
    rows, depth = 2 * parts[0][0].shape[0], parts[0][0].shape[1]
    slots = order.shape[0]
    width = sum(w.shape[1] for w in weights)
    return pl.pallas_call(
        functools.partial(project_kernel, places, heads),
        out_shape=(
            jax.ShapeDtypeStruct((rows, heads * VALUE_DIM), f32),
            jax.ShapeDtypeStruct((rows, heads * MEM_DIM), bf16),
            jax.ShapeDtypeStruct((rows, LANES), f32),
        ),
        in_specs=[SMEM, SMEM] + [ANY] * len(parts) + [HBM] * len(weights) + [VMEM, VMEM],
        out_specs=(VMEM, VMEM, VMEM),
        scratch_shapes=[
            pltpu.VMEM((slots, rows, depth), bf16),
            pltpu.VMEM((slots, depth, width), bf16),
            pltpu.VMEM((rows, width), f32),
            pltpu.SemaphoreType.DMA((len(parts),)),
            pltpu.SemaphoreType.DMA((slots, len(weights))),
        ],
        compiler_params=pltpu.CompilerParams(vmem_limit_bytes=40 * 1024 * 1024),
        cost_estimate=pl.CostEstimate(
            flops=2 * rows * depth * slots * width, bytes_accessed=0, transcendentals=0
        ),
        name="project_retain",
    )(order, rates, *[p[0] for p in parts], *weights, *tables)


def fetch_kernel(index, store, *refs):
    outs, sems = refs[:-1], refs[-1]
    copies = []
    for out in outs:
        for i in range(out.shape[0]):
            at = len(copies)
            copies.append(pltpu.make_async_copy(store.at[index[at]], out.at[i], sems.at[at]))
    for copy in copies:
        copy.start()
    for copy in copies:
        copy.wait()


def fetch(store, index, peers):
    count = index.shape[0]
    shape = jax.ShapeDtypeStruct((count // peers,) + store.shape[1:], store.dtype)
    return pl.pallas_call(
        fetch_kernel,
        out_shape=(shape,) * peers,
        in_specs=[SMEM, ANY],
        out_specs=(VMEM,) * peers,
        scratch_shapes=[pltpu.SemaphoreType.DMA((count,))],
        name="fetch_rows",
    )(index, store)


def compact_kernel(source, index, store, *refs):
    arrived = refs[:-3]
    halves, sems = refs[-3:-1], refs[-1]
    half = halves[0].shape[0]
    for i in range(2 * half):
        out = halves[i // half].at[i % half]
        for k, ref in enumerate((store,) + tuple(arrived)):

            @pl.when(source[i] == k)
            def _():
                pltpu.make_async_copy(ref.at[index[i]], out, sems.at[i]).start()

    for i in range(2 * half):
        out = halves[i // half].at[i % half]
        pltpu.make_async_copy(store.at[0], out, sems.at[i]).wait()


def compact(store, arrived, source, index):
    count = index.shape[0]
    shape = jax.ShapeDtypeStruct((count // 2,) + store.shape[1:], store.dtype)
    return pl.pallas_call(
        compact_kernel,
        out_shape=(shape, shape),
        in_specs=[SMEM, SMEM] + [ANY] * (1 + len(arrived)),
        out_specs=(VMEM, VMEM),
        scratch_shapes=[pltpu.SemaphoreType.DMA((count,))],
        name="compact_rows",
    )(source, index, store, *arrived)


def sum_slots(places, start, order, parts, weights, acc, xs, ws, sem_x, sem_w):
    slots = ws.shape[0]
    depth = ws.shape[1]
    width = weights[0].shape[1]
    copies = [[] for _ in range(slots)]
    for p, (slot, first) in enumerate(places):
        extent = parts[p].shape[0]
        at = slot - start
        copies[at].append(
            pltpu.make_async_copy(parts[p], xs.at[at, pl.ds(first, extent)], sem_x.at[p])
        )
    for slot in range(slots):
        row = pl.multiple_of(order[slot + start] * depth, depth)
        for w, weight in enumerate(weights):
            copies[slot].append(
                pltpu.make_async_copy(
                    weight.at[pl.ds(row, depth)],
                    ws.at[slot, :, pl.ds(w * width, width)],
                    sem_w.at[slot, w],
                )
            )
    for group in copies:
        for copy in group:
            copy.start()
    for slot in range(slots):
        for copy in copies[slot]:
            copy.wait()
        acc[...] += dot(xs[slot], ws[slot])


def near_kernel(places, *refs):
    count = len(places)
    order = refs[0]
    parts = refs[1 : 1 + count]
    weights = refs[1 + count : 3 + count]
    acc, xs, ws, sem_x, sem_w = refs[3 + count :]
    acc[...] = jnp.zeros_like(acc)
    sum_slots(places, 0, order, parts, weights, acc, xs, ws, sem_x, sem_w)


def slot_scratch(parts, weights, slots):
    rows, depth = 2 * parts[0][0].shape[0], parts[0][0].shape[1]
    width = sum(w.shape[1] for w in weights)
    return [
        pltpu.VMEM((slots, rows, depth), bf16),
        pltpu.VMEM((slots, depth, width), bf16),
        pltpu.SemaphoreType.DMA((len(parts),)),
        pltpu.SemaphoreType.DMA((slots, len(weights))),
    ]


def near_passages(parts, order, weights, slots):
    places = tuple((slot, first) for _, slot, first in parts)
    rows, depth = 2 * parts[0][0].shape[0], parts[0][0].shape[1]
    width = sum(w.shape[1] for w in weights)
    return pl.pallas_call(
        functools.partial(near_kernel, places),
        out_shape=jax.ShapeDtypeStruct((rows, width), f32),
        in_specs=[SMEM] + [ANY] * len(parts) + [HBM] * len(weights),
        out_specs=VMEM,
        scratch_shapes=slot_scratch(parts, weights, slots),
        compiler_params=pltpu.CompilerParams(vmem_limit_bytes=24 * 1024 * 1024),
        cost_estimate=pl.CostEstimate(
            flops=2 * rows * depth * slots * width, bytes_accessed=0, transcendentals=0
        ),
        name="passage_near",
    )(order, *[p[0] for p in parts], *weights)


def passage_kernel(places, start, heads, picks, *refs):
    count = len(places)
    order = refs[0]
    parts = refs[1 : 1 + count]
    weights = refs[1 + count : 3 + count]
    near, query, gate, norm, lift, out, acc, xs, ws, sem_x, sem_w = refs[3 + count :]
    width = heads * MEM_DIM
    acc[...] = near[...]
    sum_slots(places, start, order, parts, weights, acc, xs, ws, sem_x, sem_w)
    block_rows = picks * PASS_ROWS
    for h in range(heads):
        lo, hi = h * MEM_DIM, (h + 1) * MEM_DIM
        k = acc[:, lo:hi]
        k = k * lax.rsqrt(jnp.mean(k * k, axis=1, keepdims=True) + norm_eps)
        k = k.astype(bf16)
        v = acc[:, width + lo : width + hi].astype(bf16)
        for b in range(query.shape[0] // BLOCK):
            top, end = b * BLOCK, (b + 1) * BLOCK
            q = query[top:end, lo:hi]
            first, last = b * block_rows, (b + 1) * block_rows
            scores = lax.dot_general(
                q, k[first:last], (((1,), (1,)), ((), ())), preferred_element_type=f32
            )
            exponent = jnp.exp(scores * MEM_DIM ** (-0.5))
            mass = jnp.sum(exponent, axis=1, keepdims=True)
            summed = dot(exponent.astype(bf16), v[first:last])
            mem_out = (summed / mass).astype(bf16)
            lifted = dot(mem_out, lift[h])
            cols = slice(h * VALUE_DIM, (h + 1) * VALUE_DIM)
            out[top:end, cols] = (
                norm[top:end, cols] + gate[top:end, h : h + 1] * lifted
            ).astype(bf16)


def passages(parts, order, weights, near, query, gate, norm, lift, picks, start):
    heads = lift.shape[0]
    places = tuple((slot, first) for _, slot, first in parts)
    rows, depth = 2 * parts[0][0].shape[0], parts[0][0].shape[1]
    slots = order.shape[0] - start
    width = sum(w.shape[1] for w in weights)
    return pl.pallas_call(
        functools.partial(passage_kernel, places, start, heads, picks),
        out_shape=jax.ShapeDtypeStruct(norm.shape, bf16),
        in_specs=[SMEM] + [ANY] * len(parts) + [HBM] * len(weights) + [VMEM] * 5,
        out_specs=VMEM,
        scratch_shapes=[pltpu.VMEM((rows, width), f32)] + slot_scratch(parts, weights, slots),
        compiler_params=pltpu.CompilerParams(vmem_limit_bytes=24 * 1024 * 1024),
        cost_estimate=pl.CostEstimate(
            flops=2 * rows * depth * slots * width, bytes_accessed=0, transcendentals=0
        ),
        name="passage_mix",
    )(order, *[p[0] for p in parts], *weights, near, query, gate, norm, lift)


def per_device(
    ring_size,
    core_count,
    tokens,
    w_query,
    w_key,
    w_value,
    w_mem_query,
    w_mem_key,
    w_mem_value,
    w_gate,
    w_lift,
    decay_rate,
    store,
    passage_ids,
):
    block_count, picks = passage_ids.shape
    request_count = block_count * picks
    group_count = lax.axis_size("st")
    capacity = max(1, 2 * request_count // group_count)
    held_count = store.shape[0]
    mine = lax.axis_index("st")

    def exchange(value, k):
        return lax.ppermute(value, "st", [(i, i ^ k) for i in range(group_count)])

    def exchange_all(values):
        return [exchange(value, k + 1) for k, value in enumerate(values)]

    wanted = passage_ids.reshape(request_count)
    owners = wanted // held_count
    held_index = wanted % held_count
    ordinal = jnp.arange(request_count, dtype=jnp.int32)
    earlier = (owners[:, None] == owners[None, :]) & (ordinal[None, :] < ordinal[:, None])
    slot_index = jnp.sum(earlier.astype(jnp.int32), axis=1)
    source = owners ^ mine
    place = source * capacity + slot_index
    selector = (
        place[:, None] == jnp.arange(group_count * capacity, dtype=jnp.int32)[None, :]
    ).astype(jnp.int32)
    outgoing = jnp.sum(selector * held_index[:, None], axis=0).reshape(group_count, capacity)
    incoming = exchange_all([outgoing[k] for k in range(1, group_count)])

    half = tokens.shape[0] // 2
    token_halves = (tokens[:half], tokens[half:])
    token_parts, order = ring_gather(token_halves, ring_size, core_count)

    fetched = fetch(store, jnp.concatenate(incoming), group_count - 1)
    arrived = exchange_all(fetched)
    rows_at = jnp.where(source == 0, held_index, slot_index)
    own_rows = compact(store, arrived, source, rows_at)
    own_rows = [x.reshape(-1, store.shape[2]) for x in own_rows]
    row_parts, _ = ring_gather(tuple(own_rows), ring_size, core_count)

    gate_wide = jnp.pad(w_gate, ((0, 0), (0, LANES - w_gate.shape[1])))
    tables = rotary_tables(tokens.shape[0])
    norm, query, gate = project(
        token_parts,
        order,
        (w_query, w_key, w_value, w_mem_query, gate_wide),
        decay_rate,
        tables,
    )
    start = order.shape[0] - core_count
    mem_weights = (w_mem_key, w_mem_value)
    near = near_passages([p for p in row_parts if p[1] < start], order, mem_weights, start)
    far = [p for p in row_parts if p[1] >= start]
    return passages(
        far, order, mem_weights, near, query, gate, norm, w_lift, picks, start
    )


def solution(mesh):
    in_specs = (
        P("st", "tp"),
        P(None, "tp"),
        P(None, "tp"),
        P(None, "tp"),
        P(None, "tp"),
        P(None, "tp"),
        P(None, "tp"),
        P(None, "tp"),
        P("tp", None, None),
        P("tp"),
        P("st", None, "tp"),
        P("st", None),
    )
    out_specs = P("st", "tp")
    core_count = 2
    ring_size = mesh.shape["tp"] // core_count
    body = functools.partial(per_device, ring_size, core_count)

    return jax.shard_map(
        body,
        mesh=mesh,
        in_specs=in_specs,
        out_specs=out_specs,
        check_vma=False,
    )
```
